32 devices in a mesh: fs: 16 (over z, y, core), tp: 2 (over x).
Axes of the slice: x: 2, y: 2, z: 4, core: 2. Of those that a mesh axis runs over, the one named last changes fastest.
Arguments:
- inputs: bfloat16 [32768, 2048], P('fs'), may hold values from -6 to 6
- key_grads: bfloat16 [32768, 1024], P('fs', 'tp'), may hold values from -0.078125 to 0.078125
- weights: float32 [2048, 1024], P('fs', 'tp'), may hold values from -6 to 6
- momentum: float32 [2048, 1024], P('fs', 'tp'), may hold values from -6 to 6
- left_stat: float32 [4, 2048, 2048], P('tp', 'fs'), may hold values from -96 to 96
- right_stat: float32 [8, 128, 128], P('tp'), may hold values from -256 to 256
- left_root: bfloat16 [4, 2048, 2048], P('tp', 'fs'), may hold values from -0.125 to 0.125
- right_root: bfloat16 [8, 128, 128], P('tp'), may hold values from -0.5 to 0.5
Outputs:
- momentum_next: float32 [2048, 1024], P('fs', 'tp')
- left_next: float32 [4, 2048, 2048], P('tp', 'fs')
- right_next: float32 [8, 128, 128], P('tp')
- update: float32 [2048, 1024], P('fs', 'tp')
- weights_next: float32 [2048, 1024], P('fs', 'tp')
- weights_copy: bfloat16 [2048, 1024], P(None, 'tp')
The draws below stay inside these ranges and needn't reach their ends.
All inputs are finite; a program needn't handle non-finite values.
Results may differ from the reference program's by a relative error of at most 0.0033.
Values may be sent and summed in bfloat16 or wider, within the bound.
A program may use at most 64 MiB of HBM per device.

```python
import jax
import jax.numpy as jnp
from jax import lax

D = 2048
HEADS = 8
HD = 128
COLBLK = 256
TOKENS = 32768
C = 1024
NBLK = 4


def with_spikes(values, rng, source, target, blocks, factor):
    def block_of(axis_at):
        return (jnp.arange(values.shape[axis_at]) // (values.shape[axis_at] // blocks)).reshape((-1,) + (1,) * (values.ndim - 1 - axis_at))

    one_side = jax.random.permutation(rng, blocks)[block_of(target)]
    second = (block_of(target) + blocks // 2) % blocks
    return jnp.where((block_of(source) == one_side) | (block_of(source) == second), factor * values, values)


def block_scale(rng, extent, cuts, least, largest):
    level, own = 1.0, jax.random.fold_in(rng, 6)
    for position, blocks in cuts:
        draws = jnp.exp(jax.random.uniform(jax.random.fold_in(own, position), (blocks,), jnp.float32, least / len(cuts), largest / len(cuts)))
        level = level * jnp.repeat(draws, extent[position] // blocks).reshape([-1 if axis == position else 1 for axis in range(len(extent))])
    return level


def centred(stream_key, dims, scale, reach, shards=(), kind=jnp.bfloat16):
    gain = block_scale(stream_key, dims, shards, -0.22, 0.18) if shards else 1.0
    array = jax.random.normal(stream_key, dims, jnp.float32) * scale * gain
    return jnp.minimum(jnp.maximum(array, -reach), reach).astype(kind)


def bell_draw_with(stream_key, extent, scale, limit, split, heavy, kind=jnp.bfloat16):
    result = scale * jax.random.normal(stream_key, extent, jnp.float32)
    if split:
        result = result * block_scale(stream_key, extent, split, -0.22, 0.18)
    return jnp.clip(with_spikes(result, jax.random.fold_in(stream_key, 3), *heavy), -limit, limit).astype(kind)


def setup_inputs(seed: int = 0) -> dict:
    key_list = jax.random.split(jax.random.key(seed), 9)
    inputs = bell_draw_with(key_list[0], (TOKENS, D), 1.0, 6.0, ((0, 16),), (0, 1, 16, 2.0))
    key_grads = centred(key_list[1], (TOKENS, C), (TOKENS ** -0.5), 0.078125, ((0, 16), (1, 2)))
    weights = centred(key_list[2], (D, C), 1.0, 6.0, ((0, 16), (1, 2)), jnp.float32)
    momentum = centred(key_list[3], (D, C), 1.0, 6.0, ((0, 16), (1, 2)), jnp.float32)
    left_stat = centred(key_list[4], (NBLK, D, D), (COLBLK ** 0.5), 96.0, ((0, 2), (1, 16)), jnp.float32)
    right_stat = centred(key_list[5], (HEADS, HD, HD), (D ** 0.5), 256.0, ((0, 2),), jnp.float32)
    left_root = centred(key_list[6], (NBLK, D, D), D ** -0.5, 0.125, ((0, 2), (1, 16)))
    right_root = centred(key_list[7], (HEADS, HD, HD), HD ** -0.5, 0.5, ((0, 2),))
    return {"inputs": inputs, "key_grads": key_grads, "weights": weights, "momentum": momentum, "left_stat": left_stat, "right_stat": right_stat, "left_root": left_root, "right_root": right_root}


def reference(inputs, key_grads, weights, momentum, left_stat, right_stat, left_root, right_root):
    grad = lax.dot_general(inputs, key_grads, (((0,), (0,)), ((), ())), preferred_element_type=jnp.float32)
    grad_bf = grad.astype(jnp.bfloat16)
    nblocks = left_root.shape[0]
    heads = right_root.shape[0]
    head_size = right_root.shape[1]
    width = grad.shape[0]
    blocks = grad_bf.astype(jnp.float32).reshape(width, nblocks, -1)
    left_part = jnp.einsum('brd,dbc->rbc', left_root.astype(jnp.float32), blocks)
    left_part = left_part.reshape(width, -1).astype(jnp.bfloat16)
    precond = jnp.einsum('rhi,hij->rhj', left_part.astype(jnp.float32).reshape(width, heads, head_size), right_root.astype(jnp.float32)).reshape(width, -1)
    left_next = 0.95 * left_stat + 0.05 * jnp.einsum('rbc,sbc->brs', blocks, blocks)
    by_head = grad_bf.astype(jnp.float32).reshape(width, heads, head_size)
    right_next = 0.95 * right_stat + 0.05 * jnp.einsum('rhi,rhj->hij', by_head, by_head)
    scale = jnp.sqrt(jnp.sum(grad * grad) / (jnp.sum(precond * precond) + 1e-06))
    momentum_next = 0.9 * momentum + scale * precond
    update = -0.25 * (momentum_next + 0.4 * weights)
    weights_next = weights + update
    return (momentum_next, left_next, right_next, update, weights_next, weights_next.astype(jnp.bfloat16))
```

```python
import functools

import jax
import jax.numpy as jnp
from jax import lax
from jax.experimental import pallas as pl
from jax.experimental.pallas import tpu as pltpu
from jax.sharding import PartitionSpec as P

MESH = pl.DeviceIdType.MESH


def plain_body(inputs, key_grads, weights, momentum, left_stat, right_stat, left_root, right_root):
    row_count = weights.shape[0]
    col_count = weights.shape[1]
    block_count = left_root.shape[0]
    head_count = right_root.shape[0]
    head_size = right_root.shape[1]
    model_width = inputs.shape[1]
    partial_grad = lax.dot_general(
        inputs, key_grads, (((0,), (0,)), ((), ())), preferred_element_type=jnp.float32
    )
    summed = lax.psum(partial_grad, "fs")
    whole_bf = summed.astype(jnp.bfloat16)
    row_offset = lax.axis_index("fs") * row_count
    grad = lax.dynamic_slice_in_dim(summed, row_offset, row_count, 0)
    own_rows = lax.dynamic_slice_in_dim(whole_bf, row_offset, row_count, 0)
    whole_blocks = whole_bf.reshape(model_width, block_count, -1)
    left_part = jnp.einsum(
        "brd,dbc->rbc", left_root, whole_blocks, preferred_element_type=jnp.float32
    ).reshape(row_count, col_count)
    row_gram = jnp.einsum(
        "rbc,dbc->brd",
        own_rows.reshape(row_count, block_count, -1),
        whole_blocks,
        preferred_element_type=jnp.float32,
    )
    whole_heads = whole_bf.reshape(model_width, head_count, head_size)
    head_gram = jnp.einsum(
        "dhi,dhj->hij", whole_heads, whole_heads, preferred_element_type=jnp.float32
    )
    left_bf = left_part.astype(jnp.bfloat16)
    precond = jnp.einsum(
        "rhi,hij->rhj",
        left_bf.reshape(row_count, head_count, head_size),
        right_root,
        preferred_element_type=jnp.float32,
    ).reshape(row_count, col_count)
    left_next = 0.95 * left_stat + 0.05 * row_gram
    right_next = 0.95 * right_stat + 0.05 * head_gram
    grad_square, precond_square = lax.psum(
        (jnp.sum(grad * grad), jnp.sum(precond * precond)), ("fs", "tp")
    )
    scale = jnp.sqrt(grad_square / (precond_square + 1e-06))
    momentum_next = 0.9 * momentum + scale * precond
    update = -0.25 * (momentum_next + 0.4 * weights)
    weights_next = weights + update
    weights_copy = lax.all_gather(weights_next.astype(jnp.bfloat16), "fs", axis=0, tiled=True)
    return (momentum_next, left_next, right_next, update, weights_next, weights_copy)


def kernel(
    fs, tp, x_hbm, g_hbm, w_hbm, m_hbm, lroot_hbm, rroot_hbm,
    step_ref, gram_ref, hgram_ref, wall_ref,
    xv, gv, wv, mv, lroot, rroot, pbuf, crecv, ysend, yrecv, zsend, zrecv, whole, acc, grad_own, sc,
    in_sem, x_sem, c_ss, c_rs, y_ss, y_rs, z_ss, z_rs, ag_ss, ag_rs, sc_ss, sc_rs,
):
    Y, Z = 2, fs // 4
    chips = Y * Z
    rows, cols = wv.shape
    blocks = lroot.shape[0]
    heads, hd = rroot.shape[0], rroot.shape[1]
    bw = cols // blocks
    f32, bf16 = jnp.float32, jnp.bfloat16
    me = lax.axis_index("fs")
    t = lax.axis_index("tp")
    c = me % 2
    y = (me // 2) % Y
    z = me // (2 * Y)

    def idx(zz, yy, cc):
        return (zz * Y + yy) * 2 + cc

    def remote(src, dst, ss, rs, peer):
        cp = pltpu.make_async_remote_copy(
            src_ref=src, dst_ref=dst, send_sem=ss, recv_sem=rs,
            device_id=(peer, t), device_id_type=MESH,
        )
        cp.start()
        return cp

    partner = idx(z, y, 1 - c)
    ypeer = idx(z, 1 - y, c)
    zpeer = [idx((z + d) % Z, y, c) for d in range(1, Z)]

    gcp = pltpu.make_async_copy(g_hbm, gv, in_sem.at[0])
    gcp.start()
    order = []
    for i in range(chips):
        yy = (y + 1 + i // Z) % Y
        zz = (z + 1 + i) % Z
        order.append(zz * Y + yy)
    xcp = []
    for i in range(chips):
        start = pl.multiple_of(order[i] * (2 * rows), 2 * rows)
        cp = pltpu.make_async_copy(x_hbm.at[:, pl.ds(start, 2 * rows)], xv.at[i], x_sem.at[i])
        cp.start()
        xcp.append(cp)
    side = []
    for k, (a, b) in enumerate(((lroot_hbm, lroot), (rroot_hbm, rroot), (w_hbm, wv), (m_hbm, mv))):
        cp = pltpu.make_async_copy(a, b, in_sem.at[k + 1])
        cp.start()
        side.append(cp)

    barrier = pltpu.get_barrier_semaphore()
    total = fs * tp
    linear = t * fs + me

    @pl.loop(1, total)
    def _(k):
        other = (linear + k) % total
        pl.semaphore_signal(
            barrier, inc=1, device_id=(other % fs, other // fs), device_id_type=MESH
        )

    pl.semaphore_wait(barrier, total - 1)

    ccp, ycp, zcp = [], [], []

    def combine(i):
        ccp[i].wait_recv()
        s = pbuf[i, c] + crecv[i]
        if i < Z:
            ysend[i] = s.astype(bf16)
            ycp.append(remote(ysend.at[i], yrecv.at[i], y_ss.at[i], y_rs.at[i], ypeer))
        else:
            crecv[i] = s

    def zstage(j):
        ycp[j].wait_recv()
        s = crecv[Z + j] + yrecv[j].astype(f32)
        if j < Z - 1:
            zsend[j] = s.astype(bf16)
            zcp.append(remote(zsend.at[j], zrecv.at[j], z_ss.at[j], z_rs.at[j], zpeer[j]))
        else:
            for k in range(Z - 1):
                zcp[k].wait_recv()
                s = s + zrecv[k].astype(f32)
            grad_own[...] = s
            whole[me] = s.astype(bf16)

    gcp.wait()
    for i in range(chips):
        xcp[i].wait()
        for half in range(2):
            pbuf[i, half] = lax.dot_general(
                xv[i, :, half * rows:(half + 1) * rows], gv[...],
                (((0,), (0,)), ((), ())), preferred_element_type=f32,
            )
        ccp.append(remote(pbuf.at[i, 1 - c], crecv.at[i], c_ss.at[i], c_rs.at[i], partner))
        if i > 0:
            combine(i - 1)
    combine(chips - 1)
    for j in range(Z):
        zstage(j)

    def gather(buf, phase, use):
        sends = []

        def send(f, slot, peer):
            cp = remote(buf.at[f], buf.at[f], ag_ss.at[phase, slot], ag_rs.at[phase, slot], peer)
            sends.append(cp)

        def arrived(f, slot):
            pltpu.make_async_remote_copy(
                src_ref=buf.at[f], dst_ref=buf.at[f], send_sem=ag_ss.at[phase, slot],
                recv_sem=ag_rs.at[phase, slot], device_id=(ypeer, t), device_id_type=MESH,
            ).wait_recv()

        y0, c0 = Z - 1, 2 * Z - 1
        send(me, y0, ypeer)
        for d in range(1, Z):
            send(me, d - 1, zpeer[d - 1])
        send(me, c0, partner)
        use(me)
        for d in range(1, Z):
            f = idx((z + Z - d) % Z, y, c)
            arrived(f, d - 1)
            send(f, y0 + d, ypeer)
            send(f, c0 + d, partner)
            use(f)
        for d in range(Z):
            f = idx((z + Z - d) % Z, 1 - y, c)
            arrived(f, y0 + d)
            send(f, c0 + Z + d, partner)
            use(f)
        for k in range(2 * Z):
            yy = y if k < Z else 1 - y
            f = idx((z + Z - k) % Z, yy, 1 - c)
            arrived(f, c0 + k)
            use(f)
        for cp in sends:
            cp.wait_send()

    for cp in side:
        cp.wait()
    acc[...] = jnp.zeros_like(acc)

    def use_grad(f):
        at = pl.ds(pl.multiple_of(f * rows, rows), rows)
        for b in range(blocks):
            acc[:, b * bw:(b + 1) * bw] += jnp.dot(
                lroot[b, :, at], whole[f, :, b * bw:(b + 1) * bw], preferred_element_type=f32
            )

    gather(whole, 0, use_grad)

    for h in range(heads):
        part = acc[:, h * hd:(h + 1) * hd].astype(bf16)
        step_ref[:, h * hd:(h + 1) * hd] = jnp.dot(part, rroot[h], preferred_element_type=f32)
    g = grad_own[...]
    p = step_ref[...]
    line = lax.broadcasted_iota(jnp.int32, sc.shape[1:], 0)
    sc[linear] = jnp.where(line < 4, jnp.sum(g * g), jnp.sum(p * p))

    def scalar_copy(k):
        other = (linear + k) % total
        return pltpu.make_async_remote_copy(
            src_ref=sc.at[linear], dst_ref=sc.at[linear], send_sem=sc_ss.at[k],
            recv_sem=sc_rs.at[k], device_id=(other % fs, other // fs), device_id_type=MESH,
        )

    @pl.loop(1, total)
    def _(k):
        scalar_copy(k).start()

    hgram_ref[...] = jnp.zeros_like(hgram_ref)

    @pl.loop(0, fs)
    def _(f):
        at = pl.ds(pl.multiple_of(f * rows, rows), rows)
        for b in range(blocks):
            gram_ref[b, :, at] = lax.dot_general(
                whole[me, :, b * bw:(b + 1) * bw], whole[f, :, b * bw:(b + 1) * bw],
                (((1,), (1,)), ((), ())), preferred_element_type=f32,
            )
        for h in range(heads):
            v = whole[f, :, h * hd:(h + 1) * hd]
            hgram_ref[h] += lax.dot_general(
                v, v, (((0,), (0,)), ((), ())), preferred_element_type=f32
            )

    @pl.loop(1, total)
    def _(k):
        scalar_copy(k).wait()

    sums = jnp.sum(sc[...], axis=0)
    scale = jnp.sqrt(sums[0:1, 0:1] / (sums[4:5, 0:1] + 1e-06))
    step = scale * step_ref[...]
    step_ref[...] = step
    w = wv[...]
    wall_ref[me] = (w - 0.25 * ((0.9 * mv[...] + step) + 0.4 * w)).astype(bf16)
    gather(wall_ref, 1, lambda f: None)
    for cp in ccp + ycp + zcp:
        cp.wait_send()


def fast_body(fs, tp, inputs, key_grads, weights, momentum, left_stat, right_stat, left_root, right_root):
    rows, cols = weights.shape
    tokens, width = inputs.shape
    blocks = left_root.shape[0]
    Y, Z = 2, fs // 4
    chips = Y * Z
    f32, bf16 = jnp.float32, jnp.bfloat16
    vm = pltpu.VMEM
    dma = pltpu.SemaphoreType.DMA
    step, gram, hgram, wall = pl.pallas_call(
        functools.partial(kernel, fs, tp),
        out_shape=(
            jax.ShapeDtypeStruct((rows, cols), f32),
            jax.ShapeDtypeStruct((blocks, rows, width), f32),
            jax.ShapeDtypeStruct(right_root.shape, f32),
            jax.ShapeDtypeStruct((fs, rows, cols), bf16),
        ),
        in_specs=[pl.BlockSpec(memory_space=pl.ANY)] * 6,
        out_specs=[pl.BlockSpec(memory_space=pltpu.VMEM)] * 4,
        scratch_shapes=[
            vm((chips, tokens, 2 * rows), bf16),
            vm((tokens, cols), bf16),
            vm((rows, cols), f32),
            vm((rows, cols), f32),
            vm(left_root.shape, bf16),
            vm(right_root.shape, bf16),
            vm((chips, 2, rows, cols), f32),
            vm((chips, rows, cols), f32),
            vm((Z, rows, cols), bf16),
            vm((Z, rows, cols), bf16),
            vm((Z - 1, rows, cols), bf16),
            vm((Z - 1, rows, cols), bf16),
            vm((fs, rows, cols), bf16),
            vm((rows, cols), f32),
            vm((rows, cols), f32),
            vm((fs * tp, 8, 128), f32),
            dma((5,)), dma((chips,)),
            dma((chips,)), dma((chips,)),
            dma((Z,)), dma((Z,)),
            dma((Z - 1,)), dma((Z - 1,)),
            dma((2, 4 * Z - 1)), dma((2, 4 * Z - 1)),
            dma((fs * tp,)), dma((fs * tp,)),
        ],
        compiler_params=pltpu.CompilerParams(
            collective_id=0, has_side_effects=True, vmem_limit_bytes=56 * 1024 * 1024
        ),
    )(inputs, key_grads, weights, momentum, left_root, right_root)
    left_next = 0.95 * left_stat + 0.05 * gram
    right_next = 0.95 * right_stat + 0.05 * hgram
    momentum_next = 0.9 * momentum + step
    update = -0.25 * (momentum_next + 0.4 * weights)
    weights_next = weights + update
    weights_copy = wall.reshape(width, cols)
    return (momentum_next, left_next, right_next, update, weights_next, weights_copy)


def solution(mesh):
    fs, tp = mesh.shape["fs"], mesh.shape["tp"]
    in_specs = (
        P("fs", None),
        P("fs", "tp"),
        P("fs", "tp"),
        P("fs", "tp"),
        P("tp", "fs", None),
        P("tp", None, None),
        P("tp", "fs", None),
        P("tp", None, None),
    )
    out_specs = (
        P("fs", "tp"),
        P("tp", "fs", None),
        P("tp", None, None),
        P("fs", "tp"),
        P("fs", "tp"),
        P(None, "tp"),
    )

    def body(inputs, *rest):
        rows = inputs.shape[1] // fs
        if fs % 4 == 0 and fs >= 8 and rows % 128 == 0:
            return fast_body(fs, tp, inputs, *rest)
        return plain_body(inputs, *rest)

    return jax.shard_map(body, mesh=mesh, in_specs=in_specs, out_specs=out_specs, check_vma=False)
```

```python
import functools

import jax
import jax.numpy as jnp
from jax import lax
from jax.experimental import pallas as pl
from jax.experimental.pallas import tpu as pltpu
from jax.sharding import PartitionSpec as P

MESH = pl.DeviceIdType.MESH


def plain_body(inputs, key_grads, weights, momentum, left_stat, right_stat, left_root, right_root):
    row_count = weights.shape[0]
    col_count = weights.shape[1]
    block_count = left_root.shape[0]
    head_count = right_root.shape[0]
    head_size = right_root.shape[1]
    model_width = inputs.shape[1]
    partial_grad = lax.dot_general(
        inputs, key_grads, (((0,), (0,)), ((), ())), preferred_element_type=jnp.float32
    )
    summed = lax.psum(partial_grad, "fs")
    whole_bf = summed.astype(jnp.bfloat16)
    row_offset = lax.axis_index("fs") * row_count
    grad = lax.dynamic_slice_in_dim(summed, row_offset, row_count, 0)
    own_rows = lax.dynamic_slice_in_dim(whole_bf, row_offset, row_count, 0)
    whole_blocks = whole_bf.reshape(model_width, block_count, -1)
    left_part = jnp.einsum(
        "brd,dbc->rbc", left_root, whole_blocks, preferred_element_type=jnp.float32
    ).reshape(row_count, col_count)
    row_gram = jnp.einsum(
        "rbc,dbc->brd",
        own_rows.reshape(row_count, block_count, -1),
        whole_blocks,
        preferred_element_type=jnp.float32,
    )
    whole_heads = whole_bf.reshape(model_width, head_count, head_size)
    head_gram = jnp.einsum(
        "dhi,dhj->hij", whole_heads, whole_heads, preferred_element_type=jnp.float32
    )
    left_bf = left_part.astype(jnp.bfloat16)
    precond = jnp.einsum(
        "rhi,hij->rhj",
        left_bf.reshape(row_count, head_count, head_size),
        right_root,
        preferred_element_type=jnp.float32,
    ).reshape(row_count, col_count)
    left_next = 0.95 * left_stat + 0.05 * row_gram
    right_next = 0.95 * right_stat + 0.05 * head_gram
    grad_square, precond_square = lax.psum(
        (jnp.sum(grad * grad), jnp.sum(precond * precond)), ("fs", "tp")
    )
    scale = jnp.sqrt(grad_square / (precond_square + 1e-06))
    momentum_next = 0.9 * momentum + scale * precond
    update = -0.25 * (momentum_next + 0.4 * weights)
    weights_next = weights + update
    weights_copy = lax.all_gather(weights_next.astype(jnp.bfloat16), "fs", axis=0, tiled=True)
    return (momentum_next, left_next, right_next, update, weights_next, weights_copy)


def kernel(
    fs, tp, x_hbm, g_hbm, w_hbm, m_hbm, lroot_hbm, rroot_hbm,
    step_ref, gram_ref, hgram_ref, wall_ref,
    xv, gv, wv, mv, lroot, rroot, pbuf, crecv, ysend, yrecv, zsend, zrecv, whole, acc, grad_own, sc,
    in_sem, x_sem, c_ss, c_rs, y_ss, y_rs, z_ss, z_rs, gu_ss, gd_ss, gz_rs, gy_ss, gy_rs, gc_ss, gc_rs, sc_ss, sc_rs,
):
    Y, Z = 2, fs // 4
    chips = Y * Z
    rows, cols = wv.shape
    blocks = lroot.shape[0]
    heads, hd = rroot.shape[0], rroot.shape[1]
    bw = cols // blocks
    f32, bf16 = jnp.float32, jnp.bfloat16
    me = lax.axis_index("fs")
    t = lax.axis_index("tp")
    c = me % 2
    y = (me // 2) % Y
    z = me // (2 * Y)

    def idx(zz, yy, cc):
        return (zz * Y + yy) * 2 + cc

    def remote(src, dst, ss, rs, peer):
        cp = pltpu.make_async_remote_copy(
            src_ref=src, dst_ref=dst, send_sem=ss, recv_sem=rs,
            device_id=(peer, t), device_id_type=MESH,
        )
        cp.start()
        return cp

    partner = idx(z, y, 1 - c)
    ypeer = idx(z, 1 - y, c)
    zpeer = [idx((z + d) % Z, y, c) for d in range(1, Z)]

    gcp = pltpu.make_async_copy(g_hbm, gv, in_sem.at[0])
    gcp.start()
    order = []
    for i in range(chips):
        yy = (y + 1 + i // Z) % Y
        zz = (z + 1 + i) % Z
        order.append(zz * Y + yy)
    xcp = []
    for i in range(chips):
        start = pl.multiple_of(order[i] * (2 * rows), 2 * rows)
        cp = pltpu.make_async_copy(x_hbm.at[:, pl.ds(start, 2 * rows)], xv.at[i], x_sem.at[i])
        cp.start()
        xcp.append(cp)
    side = []
    for k, (a, b) in enumerate(((lroot_hbm, lroot), (rroot_hbm, rroot), (w_hbm, wv), (m_hbm, mv))):
        cp = pltpu.make_async_copy(a, b, in_sem.at[k + 1])
        cp.start()
        side.append(cp)

    barrier = pltpu.get_barrier_semaphore()
    total = fs * tp
    linear = t * fs + me

    @pl.loop(1, total)
    def _(k):
        other = (linear + k) % total
        pl.semaphore_signal(
            barrier, inc=1, device_id=(other % fs, other // fs), device_id_type=MESH
        )

    ccp, ycp, zcp = [], [], []

    def combine(i):
        ccp[i].wait_recv()
        s = pbuf[i, c] + crecv[i]
        if i < Z:
            ysend[i] = s.astype(bf16)
            ycp.append(remote(ysend.at[i], yrecv.at[i], y_ss.at[i], y_rs.at[i], ypeer))
        else:
            crecv[i] = s

    def zstage(j):
        ycp[j].wait_recv()
        s = crecv[Z + j] + yrecv[j].astype(f32)
        if j < Z - 1:
            zsend[j] = s.astype(bf16)
            zcp.append(remote(zsend.at[j], zrecv.at[j], z_ss.at[j], z_rs.at[j], zpeer[j]))
        else:
            for k in range(Z - 1):
                zcp[k].wait_recv()
                s = s + zrecv[k].astype(f32)
            grad_own[...] = s
            whole[me] = s.astype(bf16)

    gcp.wait()
    for i in range(chips):
        xcp[i].wait()
        for half in range(2):
            pbuf[i, half] = lax.dot_general(
                xv[i, :, half * rows:(half + 1) * rows], gv[...],
                (((0,), (0,)), ((), ())), preferred_element_type=f32,
            )
        if i == 0:
            pl.semaphore_wait(barrier, total - 1)
        ccp.append(remote(pbuf.at[i, 1 - c], crecv.at[i], c_ss.at[i], c_rs.at[i], partner))
        if i > 0:
            combine(i - 1)
    combine(chips - 1)
    for j in range(Z):
        zstage(j)

    hr = rows // 2
    halves = range(2)

    def gather(buf, ph, use, filler):
        def copy(kind, q, h):
            if kind == "c":
                f, peer, ss, rs = 2 * q + c, partner, gc_ss, gc_rs
            elif kind == "y":
                f, peer, ss, rs = idx(q, y, c), ypeer, gy_ss, gy_rs
            else:
                up = kind == "u"
                f, peer = idx(q, y, c), idx(lax.rem(z + (1 if up else Z - 1), Z), y, c)
                ss, rs = gu_ss if up else gd_ss, gz_rs
            part = buf.at[f, pl.ds(h * hr, hr)]
            return pltpu.make_async_remote_copy(
                src_ref=part, dst_ref=part, send_sem=ss.at[ph, h, q], recv_sem=rs.at[ph, h, q],
                device_id=(peer, t), device_id_type=MESH,
            )

        def arrived(kind, q, h):
            if kind == "c":
                f, ss, rs = 2 * q + 1 - c, gc_ss, gc_rs
            elif kind == "y":
                f, ss, rs = idx(q, 1 - y, c), gy_ss, gy_rs
            else:
                f, ss, rs = idx(q, y, c), gu_ss, gz_rs
            part = buf.at[f, pl.ds(h * hr, hr)]
            pltpu.make_async_remote_copy(
                src_ref=part, dst_ref=part, send_sem=ss.at[ph, h, q], recv_sem=rs.at[ph, h, q],
                device_id=(partner, t), device_id_type=MESH,
            ).wait_recv()

        def spread(q, h, up, down):
            if up:
                @pl.when(z < Z - 1)
                def _():
                    copy("u", q, h).start()
            if down:
                @pl.when(z > 0)
                def _():
                    copy("d", q, h).start()
            copy("y", q, h).start()
            copy("c", q * Y + y, h).start()

        for h in halves:
            spread(z, h, True, True)
        use(me)
        filler(0)
        for j in range(1, Z):
            for below in (True, False):
                @pl.when(z - j >= 0 if below else z + j < Z)
                def _(j=j, below=below):
                    q = z - j if below else z + j
                    for h in halves:
                        arrived("z", q, h)
                        spread(q, h, below, not below)
                    use(idx(q, y, c))
            filler(j)
        for j in range(Z):
            q = (z + j) % Z
            for h in halves:
                arrived("y", q, h)
                copy("c", q * Y + 1 - y, h).start()
            use(idx(q, 1 - y, c))
        for j in range(Z):
            for yy in (y, 1 - y):
                q = (z + j) % Z * Y + yy
                for h in halves:
                    arrived("c", q, h)
                use(2 * q + 1 - c)
        for h in halves:
            for q in range(Z):
                @pl.when((z < Z - 1) & (q <= z))
                def _(q=q, h=h):
                    copy("u", q, h).wait_send()

                @pl.when((z > 0) & (q >= z))
                def _(q=q, h=h):
                    copy("d", q, h).wait_send()

                copy("y", q, h).wait_send()
            for q in range(chips):
                copy("c", q, h).wait_send()

    for cp in side:
        cp.wait()
    acc[...] = jnp.zeros_like(acc)

    def use_grad(f):
        at = pl.ds(pl.multiple_of(f * rows, rows), rows)
        for b in range(blocks):
            acc[:, b * bw:(b + 1) * bw] += jnp.dot(
                lroot[b, :, at], whole[f, :, b * bw:(b + 1) * bw], preferred_element_type=f32
            )

    gather(whole, 0, use_grad, lambda j: None)

    for h in range(heads):
        part = acc[:, h * hd:(h + 1) * hd].astype(bf16)
        step_ref[:, h * hd:(h + 1) * hd] = jnp.dot(part, rroot[h], preferred_element_type=f32)
    g = grad_own[...]
    p = step_ref[...]
    line = lax.broadcasted_iota(jnp.int32, sc.shape[1:], 0)
    sc[linear] = jnp.where(line < 4, jnp.sum(g * g), jnp.sum(p * p))

    def scalar_copy(k):
        other = (linear + k) % total
        return pltpu.make_async_remote_copy(
            src_ref=sc.at[linear], dst_ref=sc.at[linear], send_sem=sc_ss.at[k],
            recv_sem=sc_rs.at[k], device_id=(other % fs, other // fs), device_id_type=MESH,
        )

    @pl.loop(1, total)
    def _(k):
        scalar_copy(k).start()

    hgram_ref[...] = jnp.zeros_like(hgram_ref)

    def grams(j):
        @pl.loop(j * (fs // Z), (j + 1) * (fs // Z))
        def _(f):
            at = pl.ds(pl.multiple_of(f * rows, rows), rows)
            for b in range(blocks):
                gram_ref[b, :, at] = lax.dot_general(
                    whole[me, :, b * bw:(b + 1) * bw], whole[f, :, b * bw:(b + 1) * bw],
                    (((1,), (1,)), ((), ())), preferred_element_type=f32,
                )
            for h in range(heads):
                v = whole[f, :, h * hd:(h + 1) * hd]
                hgram_ref[h] += lax.dot_general(
                    v, v, (((0,), (0,)), ((), ())), preferred_element_type=f32
                )

    @pl.loop(1, total)
    def _(k):
        scalar_copy(k).wait()

    sums = jnp.sum(sc[...], axis=0)
    scale = jnp.sqrt(sums[0:1, 0:1] / (sums[4:5, 0:1] + 1e-06))
    step = scale * step_ref[...]
    step_ref[...] = step
    w = wv[...]
    wall_ref[me] = (w - 0.25 * ((0.9 * mv[...] + step) + 0.4 * w)).astype(bf16)
    gather(wall_ref, 1, lambda f: None, grams)
    for cp in ccp + ycp + zcp:
        cp.wait_send()


def fast_body(fs, tp, inputs, key_grads, weights, momentum, left_stat, right_stat, left_root, right_root):
    rows, cols = weights.shape
    tokens, width = inputs.shape
    blocks = left_root.shape[0]
    Y, Z = 2, fs // 4
    chips = Y * Z
    f32, bf16 = jnp.float32, jnp.bfloat16
    vm = pltpu.VMEM
    dma = pltpu.SemaphoreType.DMA
    step, gram, hgram, wall = pl.pallas_call(
        functools.partial(kernel, fs, tp),
        out_shape=(
            jax.ShapeDtypeStruct((rows, cols), f32),
            jax.ShapeDtypeStruct((blocks, rows, width), f32),
            jax.ShapeDtypeStruct(right_root.shape, f32),
            jax.ShapeDtypeStruct((fs, rows, cols), bf16),
        ),
        in_specs=[pl.BlockSpec(memory_space=pltpu.HBM)] * 6,
        out_specs=[pl.BlockSpec(memory_space=pltpu.VMEM)] * 4,
        scratch_shapes=[
            vm((chips, tokens, 2 * rows), bf16),
            vm((tokens, cols), bf16),
            vm((rows, cols), f32),
            vm((rows, cols), f32),
            vm(left_root.shape, bf16),
            vm(right_root.shape, bf16),
            vm((chips, 2, rows, cols), f32),
            vm((chips, rows, cols), f32),
            vm((Z, rows, cols), bf16),
            vm((Z, rows, cols), bf16),
            vm((Z - 1, rows, cols), bf16),
            vm((Z - 1, rows, cols), bf16),
            vm((fs, rows, cols), bf16),
            vm((rows, cols), f32),
            vm((rows, cols), f32),
            vm((fs * tp, 8, 128), f32),
            dma((5,)), dma((chips,)),
            dma((chips,)), dma((chips,)),
            dma((Z,)), dma((Z,)),
            dma((Z - 1,)), dma((Z - 1,)),
            dma((2, 2, Z)), dma((2, 2, Z)), dma((2, 2, Z)),
            dma((2, 2, Z)), dma((2, 2, Z)),
            dma((2, 2, chips)), dma((2, 2, chips)),
            dma((fs * tp,)), dma((fs * tp,)),
        ],
        compiler_params=pltpu.CompilerParams(
            collective_id=0, has_side_effects=True, vmem_limit_bytes=30 * 1024 * 1024
        ),
    )(inputs, key_grads, weights, momentum, left_root, right_root)
    left_next = 0.95 * left_stat + 0.05 * gram
    right_next = 0.95 * right_stat + 0.05 * hgram
    momentum_next = 0.9 * momentum + step
    update = -0.25 * (momentum_next + 0.4 * weights)
    weights_next = weights + update
    weights_copy = wall.reshape(width, cols)
    return (momentum_next, left_next, right_next, update, weights_next, weights_copy)


def solution(mesh):
    fs, tp = mesh.shape["fs"], mesh.shape["tp"]
    in_specs = (
        P("fs", None),
        P("fs", "tp"),
        P("fs", "tp"),
        P("fs", "tp"),
        P("tp", "fs", None),
        P("tp", None, None),
        P("tp", "fs", None),
        P("tp", None, None),
    )
    out_specs = (
        P("fs", "tp"),
        P("tp", "fs", None),
        P("tp", None, None),
        P("fs", "tp"),
        P("fs", "tp"),
        P(None, "tp"),
    )

    def body(inputs, *rest):
        rows = inputs.shape[1] // fs
        if fs % 4 == 0 and fs >= 8 and rows % 128 == 0:
            return fast_body(fs, tp, inputs, *rest)
        return plain_body(inputs, *rest)

    return jax.shard_map(body, mesh=mesh, in_specs=in_specs, out_specs=out_specs, check_vma=False)
```

```python
import functools

import jax
import jax.numpy as jnp
from jax import lax
from jax.experimental import pallas as pl
from jax.experimental.pallas import tpu as pltpu
from jax.sharding import PartitionSpec as P

MESH = pl.DeviceIdType.MESH


def plain_body(inputs, key_grads, weights, momentum, left_stat, right_stat, left_root, right_root):
    row_count = weights.shape[0]
    col_count = weights.shape[1]
    block_count = left_root.shape[0]
    head_count = right_root.shape[0]
    head_size = right_root.shape[1]
    model_width = inputs.shape[1]
    partial_grad = lax.dot_general(
        inputs, key_grads, (((0,), (0,)), ((), ())), preferred_element_type=jnp.float32
    )
    summed = lax.psum(partial_grad, "fs")
    whole_bf = summed.astype(jnp.bfloat16)
    row_offset = lax.axis_index("fs") * row_count
    grad = lax.dynamic_slice_in_dim(summed, row_offset, row_count, 0)
    own_rows = lax.dynamic_slice_in_dim(whole_bf, row_offset, row_count, 0)
    whole_blocks = whole_bf.reshape(model_width, block_count, -1)
    left_part = jnp.einsum(
        "brd,dbc->rbc", left_root, whole_blocks, preferred_element_type=jnp.float32
    ).reshape(row_count, col_count)
    row_gram = jnp.einsum(
        "rbc,dbc->brd",
        own_rows.reshape(row_count, block_count, -1),
        whole_blocks,
        preferred_element_type=jnp.float32,
    )
    whole_heads = whole_bf.reshape(model_width, head_count, head_size)
    head_gram = jnp.einsum(
        "dhi,dhj->hij", whole_heads, whole_heads, preferred_element_type=jnp.float32
    )
    left_bf = left_part.astype(jnp.bfloat16)
    precond = jnp.einsum(
        "rhi,hij->rhj",
        left_bf.reshape(row_count, head_count, head_size),
        right_root,
        preferred_element_type=jnp.float32,
    ).reshape(row_count, col_count)
    left_next = 0.95 * left_stat + 0.05 * row_gram
    right_next = 0.95 * right_stat + 0.05 * head_gram
    grad_square, precond_square = lax.psum(
        (jnp.sum(grad * grad), jnp.sum(precond * precond)), ("fs", "tp")
    )
    scale = jnp.sqrt(grad_square / (precond_square + 1e-06))
    momentum_next = 0.9 * momentum + scale * precond
    update = -0.25 * (momentum_next + 0.4 * weights)
    weights_next = weights + update
    weights_copy = lax.all_gather(weights_next.astype(jnp.bfloat16), "fs", axis=0, tiled=True)
    return (momentum_next, left_next, right_next, update, weights_next, weights_copy)


def kernel(
    fs, tp, x_hbm, g_hbm, w_hbm, m_hbm, lroot_hbm, rroot_hbm,
    step_ref, gram_ref, hgram_ref, wall_ref,
    xv, gv, wv, mv, lroot, rroot, pbuf, crecv, ysend, yrecv, zsend, zrecv, whole, acc, grad_own, sc,
    in_sem, x_sem, c_ss, c_rs, y_ss, y_rs, z_ss, z_rs, gu_ss, gd_ss, gz_rs, gy_ss, gy_rs, gc_ss, gc_rs, sc_ss, sc_rs,
):
    Y, Z = 2, fs // 4
    chips = Y * Z
    rows, cols = wv.shape
    blocks = lroot.shape[0]
    heads, hd = rroot.shape[0], rroot.shape[1]
    bw = cols // blocks
    f32, bf16 = jnp.float32, jnp.bfloat16
    me = lax.axis_index("fs")
    t = lax.axis_index("tp")
    c = me % 2
    y = (me // 2) % Y
    z = me // (2 * Y)

    def idx(zz, yy, cc):
        return (zz * Y + yy) * 2 + cc

    def remote(src, dst, ss, rs, peer):
        cp = pltpu.make_async_remote_copy(
            src_ref=src, dst_ref=dst, send_sem=ss, recv_sem=rs,
            device_id=(peer, t), device_id_type=MESH,
        )
        cp.start()
        return cp

    partner = idx(z, y, 1 - c)
    ypeer = idx(z, 1 - y, c)
    zpeer = [idx((z + d) % Z, y, c) for d in range(1, Z)]

    gcp = pltpu.make_async_copy(g_hbm, gv, in_sem.at[0])
    gcp.start()
    order = []
    for i in range(chips):
        yy = (y + 1 + i // Z) % Y
        zz = (z + 1 + i) % Z
        order.append(zz * Y + yy)
    xcp = []
    for i in range(chips):
        start = pl.multiple_of(order[i] * (2 * rows), 2 * rows)
        cp = pltpu.make_async_copy(x_hbm.at[:, pl.ds(start, 2 * rows)], xv.at[i], x_sem.at[i])
        cp.start()
        xcp.append(cp)
    side = []
    for k, (a, b) in enumerate(((lroot_hbm, lroot), (rroot_hbm, rroot), (w_hbm, wv), (m_hbm, mv))):
        cp = pltpu.make_async_copy(a, b, in_sem.at[k + 1])
        cp.start()
        side.append(cp)

    barrier = pltpu.get_barrier_semaphore()
    total = fs * tp
    linear = t * fs + me

    @pl.loop(1, total)
    def _(k):
        other = (linear + k) % total
        pl.semaphore_signal(
            barrier, inc=1, device_id=(other % fs, other // fs), device_id_type=MESH
        )

    ccp, ycp, zcp = [], [], []

    def combine(i):
        ccp[i].wait_recv()
        s = pbuf[i, c] + crecv[i]
        if i < Z:
            ysend[i] = s.astype(bf16)
            ycp.append(remote(ysend.at[i], yrecv.at[i], y_ss.at[i], y_rs.at[i], ypeer))
        else:
            crecv[i] = s

    def zstage(j):
        ycp[j].wait_recv()
        s = crecv[Z + j] + yrecv[j].astype(f32)
        if j < Z - 1:
            zsend[j] = s.astype(bf16)
            zcp.append(remote(zsend.at[j], zrecv.at[j], z_ss.at[j], z_rs.at[j], zpeer[j]))
        else:
            for k in range(Z - 1):
                zcp[k].wait_recv()
                s = s + zrecv[k].astype(f32)
            grad_own[...] = s
            whole[me] = s.astype(bf16)

    gcp.wait()
    for i in range(chips):
        xcp[i].wait()
        for half in range(2):
            pbuf[i, half] = lax.dot_general(
                xv[i, :, half * rows:(half + 1) * rows], gv[...],
                (((0,), (0,)), ((), ())), preferred_element_type=f32,
            )
        if i == 0:
            pl.semaphore_wait(barrier, total - 1)
        ccp.append(remote(pbuf.at[i, 1 - c], crecv.at[i], c_ss.at[i], c_rs.at[i], partner))
        if i > 0:
            combine(i - 1)
    combine(chips - 1)
    for j in range(Z):
        zstage(j)

    hr = rows // 2
    halves = range(2)

    def gather(buf, ph, use, filler):
        def copy(kind, q, h):
            if kind == "c":
                f, peer, ss, rs = 2 * q + c, partner, gc_ss, gc_rs
            elif kind == "y":
                f, peer, ss, rs = idx(q, y, c), ypeer, gy_ss, gy_rs
            else:
                up = kind == "u"
                f, peer = idx(q, y, c), idx(lax.rem(z + (1 if up else Z - 1), Z), y, c)
                ss, rs = gu_ss if up else gd_ss, gz_rs
            part = buf.at[f, pl.ds(h * hr, hr)]
            return pltpu.make_async_remote_copy(
                src_ref=part, dst_ref=part, send_sem=ss.at[ph, h, q], recv_sem=rs.at[ph, h, q],
                device_id=(peer, t), device_id_type=MESH,
            )

        def arrived(kind, q, h):
            if kind == "c":
                f, ss, rs = 2 * q + 1 - c, gc_ss, gc_rs
            elif kind == "y":
                f, ss, rs = idx(q, 1 - y, c), gy_ss, gy_rs
            else:
                f, ss, rs = idx(q, y, c), gu_ss, gz_rs
            part = buf.at[f, pl.ds(h * hr, hr)]
            pltpu.make_async_remote_copy(
                src_ref=part, dst_ref=part, send_sem=ss.at[ph, h, q], recv_sem=rs.at[ph, h, q],
                device_id=(partner, t), device_id_type=MESH,
            ).wait_recv()

        def spread(q, h, up, down):
            if up:
                @pl.when(z < Z - 1)
                def _():
                    copy("u", q, h).start()
            if down:
                @pl.when(z > 0)
                def _():
                    copy("d", q, h).start()
            copy("y", q, h).start()
            copy("c", q * Y + y, h).start()

        for h in halves:
            spread(z, h, True, True)
        use(me)
        filler(0)
        for j in range(1, Z):
            for below in (True, False):
                @pl.when(z - j >= 0 if below else z + j < Z)
                def _(j=j, below=below):
                    q = z - j if below else z + j
                    for h in halves:
                        arrived("z", q, h)
                        spread(q, h, below, not below)
                    use(idx(q, y, c))
            filler(j)
        for j in range(Z):
            q = (z + j) % Z
            for h in halves:
                arrived("y", q, h)
                copy("c", q * Y + 1 - y, h).start()
            use(idx(q, 1 - y, c))
        for j in range(Z):
            for yy in (y, 1 - y):
                q = (z + j) % Z * Y + yy
                for h in halves:
                    arrived("c", q, h)
                use(2 * q + 1 - c)
        for h in halves:
            for q in range(Z):
                @pl.when((z < Z - 1) & (q <= z))
                def _(q=q, h=h):
                    copy("u", q, h).wait_send()

                @pl.when((z > 0) & (q >= z))
                def _(q=q, h=h):
                    copy("d", q, h).wait_send()

                copy("y", q, h).wait_send()
            for q in range(chips):
                copy("c", q, h).wait_send()

    for cp in side:
        cp.wait()
    acc[...] = jnp.zeros_like(acc)

    def use_grad(f):
        at = pl.ds(pl.multiple_of(f * rows, rows), rows)
        for b in range(blocks):
            acc[:, b * bw:(b + 1) * bw] += jnp.dot(
                lroot[b, :, at], whole[f, :, b * bw:(b + 1) * bw], preferred_element_type=f32
            )

    gather(whole, 0, use_grad, lambda j: None)

    for h in range(heads):
        part = acc[:, h * hd:(h + 1) * hd].astype(bf16)
        step_ref[:, h * hd:(h + 1) * hd] = jnp.dot(part, rroot[h], preferred_element_type=f32)
    g = grad_own[...]
    p = step_ref[...]
    line = lax.broadcasted_iota(jnp.int32, sc.shape[1:], 0)
    sc[linear] = jnp.where(line < 4, jnp.sum(g * g), jnp.sum(p * p))

    def scalar_copy(k):
        other = (linear + k) % total
        return pltpu.make_async_remote_copy(
            src_ref=sc.at[linear], dst_ref=sc.at[linear], send_sem=sc_ss.at[k],
            recv_sem=sc_rs.at[k], device_id=(other % fs, other // fs), device_id_type=MESH,
        )

    @pl.loop(1, total)
    def _(k):
        scalar_copy(k).start()

    hgram_ref[...] = jnp.zeros_like(hgram_ref)

    def grams(j):
        @pl.loop(j * (fs // Z), (j + 1) * (fs // Z))
        def _(f):
            at = pl.ds(pl.multiple_of(f * rows, rows), rows)
            for b in range(blocks):
                gram_ref[b, :, at] = lax.dot_general(
                    whole[me, :, b * bw:(b + 1) * bw], whole[f, :, b * bw:(b + 1) * bw],
                    (((1,), (1,)), ((), ())), preferred_element_type=f32,
                )
            for h in range(heads):
                v = whole[f, :, h * hd:(h + 1) * hd]
                hgram_ref[h] += lax.dot_general(
                    v, v, (((0,), (0,)), ((), ())), preferred_element_type=f32
                )

    @pl.loop(1, total)
    def _(k):
        scalar_copy(k).wait()

    sums = jnp.sum(sc[...], axis=0)
    scale = jnp.sqrt(sums[0:1, 0:1] / (sums[4:5, 0:1] + 1e-06))
    step = scale * step_ref[...]
    step_ref[...] = step
    w = wv[...]
    wall_ref[me] = (w - 0.25 * ((0.9 * mv[...] + step) + 0.4 * w)).astype(bf16)
    gather(wall_ref, 1, lambda f: None, grams)
    for cp in ccp + ycp + zcp:
        cp.wait_send()


def fast_body(fs, tp, inputs, key_grads, weights, momentum, left_stat, right_stat, left_root, right_root):
    rows, cols = weights.shape
    tokens, width = inputs.shape
    blocks = left_root.shape[0]
    Y, Z = 2, fs // 4
    chips = Y * Z
    f32, bf16 = jnp.float32, jnp.bfloat16
    vm = pltpu.VMEM
    dma = pltpu.SemaphoreType.DMA
    operands = (inputs, key_grads, weights, momentum, left_root, right_root)
    step, gram, hgram, wall = pl.pallas_call(
        functools.partial(kernel, fs, tp),
        out_shape=(
            jax.ShapeDtypeStruct((rows, cols), f32),
            jax.ShapeDtypeStruct((blocks, rows, width), f32),
            jax.ShapeDtypeStruct(right_root.shape, f32),
            jax.ShapeDtypeStruct((fs, rows, cols), bf16),
        ),
        in_specs=[pl.BlockSpec(memory_space=pltpu.HBM)] * 6,
        out_specs=[pl.BlockSpec(memory_space=pltpu.VMEM)] * 4,
        scratch_shapes=[
            vm((chips, tokens, 2 * rows), bf16),
            vm((tokens, cols), bf16),
            vm((rows, cols), f32),
            vm((rows, cols), f32),
            vm(left_root.shape, bf16),
            vm(right_root.shape, bf16),
            vm((chips, 2, rows, cols), f32),
            vm((chips, rows, cols), f32),
            vm((Z, rows, cols), bf16),
            vm((Z, rows, cols), bf16),
            vm((Z - 1, rows, cols), bf16),
            vm((Z - 1, rows, cols), bf16),
            vm((fs, rows, cols), bf16),
            vm((rows, cols), f32),
            vm((rows, cols), f32),
            vm((fs * tp, 8, 128), f32),
            dma((5,)), dma((chips,)),
            dma((chips,)), dma((chips,)),
            dma((Z,)), dma((Z,)),
            dma((Z - 1,)), dma((Z - 1,)),
            dma((2, 2, Z)), dma((2, 2, Z)), dma((2, 2, Z)),
            dma((2, 2, Z)), dma((2, 2, Z)),
            dma((2, 2, chips)), dma((2, 2, chips)),
            dma((fs * tp,)), dma((fs * tp,)),
        ],
        compiler_params=pltpu.CompilerParams(
            collective_id=0, has_side_effects=True, vmem_limit_bytes=30 * 1024 * 1024
        ),
    )(*(pltpu.with_memory_space_constraint(a, pltpu.HBM) for a in operands))
    left_next = 0.95 * left_stat + 0.05 * gram
    right_next = 0.95 * right_stat + 0.05 * hgram
    momentum_next = 0.9 * momentum + step
    update = -0.25 * (momentum_next + 0.4 * weights)
    weights_next = weights + update
    weights_copy = wall.reshape(width, cols)
    return (momentum_next, left_next, right_next, update, weights_next, weights_copy)


def solution(mesh):
    fs, tp = mesh.shape["fs"], mesh.shape["tp"]
    in_specs = (
        P("fs", None),
        P("fs", "tp"),
        P("fs", "tp"),
        P("fs", "tp"),
        P("tp", "fs", None),
        P("tp", None, None),
        P("tp", "fs", None),
        P("tp", None, None),
    )
    out_specs = (
        P("fs", "tp"),
        P("tp", "fs", None),
        P("tp", None, None),
        P("fs", "tp"),
        P("fs", "tp"),
        P(None, "tp"),
    )

    def body(inputs, *rest):
        rows = inputs.shape[1] // fs
        if fs % 4 == 0 and fs >= 8 and rows % 128 == 0:
            return fast_body(fs, tp, inputs, *rest)
        return plain_body(inputs, *rest)

    return jax.shard_map(body, mesh=mesh, in_specs=in_specs, out_specs=out_specs, check_vma=False)
```

```python
import functools

import jax
import jax.numpy as jnp
from jax import lax
from jax.experimental import pallas as pl
from jax.experimental.pallas import tpu as pltpu
from jax.sharding import PartitionSpec as P

MESH = pl.DeviceIdType.MESH


def plain_body(inputs, key_grads, weights, momentum, left_stat, right_stat, left_root, right_root):
    row_count = weights.shape[0]
    col_count = weights.shape[1]
    block_count = left_root.shape[0]
    head_count = right_root.shape[0]
    head_size = right_root.shape[1]
    model_width = inputs.shape[1]
    partial_grad = lax.dot_general(
        inputs, key_grads, (((0,), (0,)), ((), ())), preferred_element_type=jnp.float32
    )
    summed = lax.psum(partial_grad, "fs")
    whole_bf = summed.astype(jnp.bfloat16)
    row_offset = lax.axis_index("fs") * row_count
    grad = lax.dynamic_slice_in_dim(summed, row_offset, row_count, 0)
    own_rows = lax.dynamic_slice_in_dim(whole_bf, row_offset, row_count, 0)
    whole_blocks = whole_bf.reshape(model_width, block_count, -1)
    left_part = jnp.einsum(
        "brd,dbc->rbc", left_root, whole_blocks, preferred_element_type=jnp.float32
    ).reshape(row_count, col_count)
    row_gram = jnp.einsum(
        "rbc,dbc->brd",
        own_rows.reshape(row_count, block_count, -1),
        whole_blocks,
        preferred_element_type=jnp.float32,
    )
    whole_heads = whole_bf.reshape(model_width, head_count, head_size)
    head_gram = jnp.einsum(
        "dhi,dhj->hij", whole_heads, whole_heads, preferred_element_type=jnp.float32
    )
    left_bf = left_part.astype(jnp.bfloat16)
    precond = jnp.einsum(
        "rhi,hij->rhj",
        left_bf.reshape(row_count, head_count, head_size),
        right_root,
        preferred_element_type=jnp.float32,
    ).reshape(row_count, col_count)
    left_next = 0.95 * left_stat + 0.05 * row_gram
    right_next = 0.95 * right_stat + 0.05 * head_gram
    grad_square, precond_square = lax.psum(
        (jnp.sum(grad * grad), jnp.sum(precond * precond)), ("fs", "tp")
    )
    scale = jnp.sqrt(grad_square / (precond_square + 1e-06))
    momentum_next = 0.9 * momentum + scale * precond
    update = -0.25 * (momentum_next + 0.4 * weights)
    weights_next = weights + update
    weights_copy = lax.all_gather(weights_next.astype(jnp.bfloat16), "fs", axis=0, tiled=True)
    return (momentum_next, left_next, right_next, update, weights_next, weights_copy)


def kernel(
    fs, tp, x_hbm, g_hbm, w_hbm, m_hbm, lroot_hbm, rroot_hbm,
    step_ref, gram_ref, hgram_ref, wall_ref,
    xv, gv, wv, mv, lroot, rroot, pbuf, crecv, ysend, yrecv, zsend, zrecv, whole, acc, grad_own, sc,
    in_sem, x_sem, c_ss, c_rs, y_ss, y_rs, z_ss, z_rs, gu_ss, gd_ss, gz_rs, gy_ss, gy_rs, gc_ss, gc_rs, sc_ss, sc_rs,
):
    Y, Z = 2, fs // 4
    chips = Y * Z
    rows, cols = wv.shape
    blocks = lroot.shape[0]
    heads, hd = rroot.shape[0], rroot.shape[1]
    bw = cols // blocks
    f32, bf16 = jnp.float32, jnp.bfloat16
    me = lax.axis_index("fs")
    t = lax.axis_index("tp")
    c = me % 2
    y = (me // 2) % Y
    z = me // (2 * Y)

    def idx(zz, yy, cc):
        return (zz * Y + yy) * 2 + cc

    def remote(src, dst, ss, rs, peer):
        cp = pltpu.make_async_remote_copy(
            src_ref=src, dst_ref=dst, send_sem=ss, recv_sem=rs,
            device_id=(peer, t), device_id_type=MESH,
        )
        cp.start()
        return cp

    partner = idx(z, y, 1 - c)
    ypeer = idx(z, 1 - y, c)
    zpeer = [idx((z + d) % Z, y, c) for d in range(1, Z)]

    gcp = pltpu.make_async_copy(g_hbm, gv, in_sem.at[0])
    gcp.start()
    order = []
    for i in range(chips):
        yy = (y + 1 + i // Z) % Y
        zz = (z + 1 + i) % Z
        order.append(zz * Y + yy)
    xcp = []
    ahead = 3
    for i in range(chips):
        start = pl.multiple_of(order[i] * (2 * rows), 2 * rows)
        cp = pltpu.make_async_copy(x_hbm.at[:, pl.ds(start, 2 * rows)], xv.at[i], x_sem.at[i])
        if i < ahead:
            cp.start()
        xcp.append(cp)
    side = []
    for k, (a, b) in enumerate(((lroot_hbm, lroot), (rroot_hbm, rroot), (w_hbm, wv), (m_hbm, mv))):
        cp = pltpu.make_async_copy(a, b, in_sem.at[k + 1])
        side.append(cp)

    barrier = pltpu.get_barrier_semaphore()
    total = fs * tp
    linear = t * fs + me

    @pl.loop(1, total)
    def _(k):
        other = (linear + k) % total
        pl.semaphore_signal(
            barrier, inc=1, device_id=(other % fs, other // fs), device_id_type=MESH
        )

    ccp, ycp, zcp = [], [], []

    def combine(i):
        ccp[i].wait_recv()
        s = pbuf[i, c] + crecv[i]
        if i < Z:
            ysend[i] = s.astype(bf16)
            ycp.append(remote(ysend.at[i], yrecv.at[i], y_ss.at[i], y_rs.at[i], ypeer))
        else:
            crecv[i] = s

    def zstage(j):
        ycp[j].wait_recv()
        s = crecv[Z + j] + yrecv[j].astype(f32)
        if j < Z - 1:
            zsend[j] = s.astype(bf16)
            zcp.append(remote(zsend.at[j], zrecv.at[j], z_ss.at[j], z_rs.at[j], zpeer[j]))
        else:
            for k in range(Z - 1):
                zcp[k].wait_recv()
                s = s + zrecv[k].astype(f32)
            grad_own[...] = s
            whole[me] = s.astype(bf16)

    gcp.wait()
    for i in range(chips):
        xcp[i].wait()
        if i + ahead < chips:
            xcp[i + ahead].start()
        both = lax.dot_general(
            xv[i], gv[...], (((0,), (0,)), ((), ())), preferred_element_type=f32
        )
        pbuf[i, 0] = both[:rows]
        pbuf[i, 1] = both[rows:]
        if i == 0:
            pl.semaphore_wait(barrier, total - 1)
        ccp.append(remote(pbuf.at[i, 1 - c], crecv.at[i], c_ss.at[i], c_rs.at[i], partner))
        if i > 0:
            combine(i - 1)
    for cp in side:
        cp.start()
    combine(chips - 1)
    for j in range(Z):
        zstage(j)

    hr = rows // 2
    halves = range(2)

    def gather(buf, ph, use, filler):
        def copy(kind, q, h):
            if kind == "c":
                f, peer, ss, rs = 2 * q + c, partner, gc_ss, gc_rs
            elif kind == "y":
                f, peer, ss, rs = idx(q, y, c), ypeer, gy_ss, gy_rs
            else:
                up = kind == "u"
                f, peer = idx(q, y, c), idx(lax.rem(z + (1 if up else Z - 1), Z), y, c)
                ss, rs = gu_ss if up else gd_ss, gz_rs
            part = buf.at[f, pl.ds(h * hr, hr)]
            return pltpu.make_async_remote_copy(
                src_ref=part, dst_ref=part, send_sem=ss.at[ph, h, q], recv_sem=rs.at[ph, h, q],
                device_id=(peer, t), device_id_type=MESH,
            )

        def arrived(kind, q, h):
            if kind == "c":
                f, ss, rs = 2 * q + 1 - c, gc_ss, gc_rs
            elif kind == "y":
                f, ss, rs = idx(q, 1 - y, c), gy_ss, gy_rs
            else:
                f, ss, rs = idx(q, y, c), gu_ss, gz_rs
            part = buf.at[f, pl.ds(h * hr, hr)]
            pltpu.make_async_remote_copy(
                src_ref=part, dst_ref=part, send_sem=ss.at[ph, h, q], recv_sem=rs.at[ph, h, q],
                device_id=(partner, t), device_id_type=MESH,
            ).wait_recv()

        def spread(q, h, up, down):
            if up:
                @pl.when(z < Z - 1)
                def _():
                    copy("u", q, h).start()
            if down:
                @pl.when(z > 0)
                def _():
                    copy("d", q, h).start()
            copy("y", q, h).start()
            copy("c", q * Y + y, h).start()

        for h in halves:
            spread(z, h, True, True)
        use(me)
        filler(0)
        for j in range(1, Z):
            for below in (True, False):
                @pl.when(z - j >= 0 if below else z + j < Z)
                def _(j=j, below=below):
                    q = z - j if below else z + j
                    for h in halves:
                        arrived("z", q, h)
                        spread(q, h, below, not below)
                    use(idx(q, y, c))
            filler(j)
        for j in range(Z):
            q = (z + j) % Z
            for h in halves:
                arrived("y", q, h)
                copy("c", q * Y + 1 - y, h).start()
            use(idx(q, 1 - y, c))
        for j in range(Z):
            for yy in (y, 1 - y):
                q = (z + j) % Z * Y + yy
                for h in halves:
                    arrived("c", q, h)
                use(2 * q + 1 - c)
        for h in halves:
            for q in range(Z):
                @pl.when((z < Z - 1) & (q <= z))
                def _(q=q, h=h):
                    copy("u", q, h).wait_send()

                @pl.when((z > 0) & (q >= z))
                def _(q=q, h=h):
                    copy("d", q, h).wait_send()

                copy("y", q, h).wait_send()
            for q in range(chips):
                copy("c", q, h).wait_send()

    for cp in side:
        cp.wait()
    acc[...] = jnp.zeros_like(acc)

    def use_grad(f):
        at = pl.ds(pl.multiple_of(f * rows, rows), rows)
        for b in range(blocks):
            acc[:, b * bw:(b + 1) * bw] += jnp.dot(
                lroot[b, :, at], whole[f, :, b * bw:(b + 1) * bw], preferred_element_type=f32
            )

    gather(whole, 0, use_grad, lambda j: None)

    for h in range(heads):
        part = acc[:, h * hd:(h + 1) * hd].astype(bf16)
        step_ref[:, h * hd:(h + 1) * hd] = jnp.dot(part, rroot[h], preferred_element_type=f32)
    g = grad_own[...]
    p = step_ref[...]
    line = lax.broadcasted_iota(jnp.int32, sc.shape[1:], 0)
    sc[linear] = jnp.where(line < 4, jnp.sum(g * g), jnp.sum(p * p))

    def scalar_copy(k):
        other = (linear + k) % total
        return pltpu.make_async_remote_copy(
            src_ref=sc.at[linear], dst_ref=sc.at[linear], send_sem=sc_ss.at[k],
            recv_sem=sc_rs.at[k], device_id=(other % fs, other // fs), device_id_type=MESH,
        )

    @pl.loop(1, total)
    def _(k):
        scalar_copy(k).start()

    hgram_ref[...] = jnp.zeros_like(hgram_ref)

    def grams(j):
        @pl.loop(j * (fs // Z), (j + 1) * (fs // Z))
        def _(f):
            at = pl.ds(pl.multiple_of(f * rows, rows), rows)
            for b in range(blocks):
                gram_ref[b, :, at] = lax.dot_general(
                    whole[me, :, b * bw:(b + 1) * bw], whole[f, :, b * bw:(b + 1) * bw],
                    (((1,), (1,)), ((), ())), preferred_element_type=f32,
                )
            for h in range(heads):
                v = whole[f, :, h * hd:(h + 1) * hd]
                hgram_ref[h] += lax.dot_general(
                    v, v, (((0,), (0,)), ((), ())), preferred_element_type=f32
                )

    @pl.loop(1, total)
    def _(k):
        scalar_copy(k).wait()

    sums = jnp.sum(sc[...], axis=0)
    scale = jnp.sqrt(sums[0:1, 0:1] / (sums[4:5, 0:1] + 1e-06))
    step = scale * step_ref[...]
    step_ref[...] = step
    w = wv[...]
    wall_ref[me] = (w - 0.25 * ((0.9 * mv[...] + step) + 0.4 * w)).astype(bf16)
    gather(wall_ref, 1, lambda f: None, grams)
    for cp in ccp + ycp + zcp:
        cp.wait_send()


def fast_body(fs, tp, inputs, key_grads, weights, momentum, left_stat, right_stat, left_root, right_root):
    rows, cols = weights.shape
    tokens, width = inputs.shape
    blocks = left_root.shape[0]
    Y, Z = 2, fs // 4
    chips = Y * Z
    f32, bf16 = jnp.float32, jnp.bfloat16
    vm = pltpu.VMEM
    dma = pltpu.SemaphoreType.DMA
    operands = (inputs, key_grads, weights, momentum, left_root, right_root)
    step, gram, hgram, wall = pl.pallas_call(
        functools.partial(kernel, fs, tp),
        out_shape=(
            jax.ShapeDtypeStruct((rows, cols), f32),
            jax.ShapeDtypeStruct((blocks, rows, width), f32),
            jax.ShapeDtypeStruct(right_root.shape, f32),
            jax.ShapeDtypeStruct((fs, rows, cols), bf16),
        ),
        in_specs=[pl.BlockSpec(memory_space=pltpu.HBM)] * 6,
        out_specs=[pl.BlockSpec(memory_space=pltpu.VMEM)] * 4,
        scratch_shapes=[
            vm((chips, tokens, 2 * rows), bf16),
            vm((tokens, cols), bf16),
            vm((rows, cols), f32),
            vm((rows, cols), f32),
            vm(left_root.shape, bf16),
            vm(right_root.shape, bf16),
            vm((chips, 2, rows, cols), f32),
            vm((chips, rows, cols), f32),
            vm((Z, rows, cols), bf16),
            vm((Z, rows, cols), bf16),
            vm((Z - 1, rows, cols), bf16),
            vm((Z - 1, rows, cols), bf16),
            vm((fs, rows, cols), bf16),
            vm((rows, cols), f32),
            vm((rows, cols), f32),
            vm((fs * tp, 8, 128), f32),
            dma((5,)), dma((chips,)),
            dma((chips,)), dma((chips,)),
            dma((Z,)), dma((Z,)),
            dma((Z - 1,)), dma((Z - 1,)),
            dma((2, 2, Z)), dma((2, 2, Z)), dma((2, 2, Z)),
            dma((2, 2, Z)), dma((2, 2, Z)),
            dma((2, 2, chips)), dma((2, 2, chips)),
            dma((fs * tp,)), dma((fs * tp,)),
        ],
        compiler_params=pltpu.CompilerParams(
            collective_id=0, has_side_effects=True, vmem_limit_bytes=30 * 1024 * 1024
        ),
    )(*(pltpu.with_memory_space_constraint(a, pltpu.HBM) for a in operands))
    left_next = 0.95 * left_stat + 0.05 * gram
    right_next = 0.95 * right_stat + 0.05 * hgram
    momentum_next = 0.9 * momentum + step
    update = -0.25 * (momentum_next + 0.4 * weights)
    weights_next = weights + update
    weights_copy = wall.reshape(width, cols)
    return (momentum_next, left_next, right_next, update, weights_next, weights_copy)


def solution(mesh):
    fs, tp = mesh.shape["fs"], mesh.shape["tp"]
    in_specs = (
        P("fs", None),
        P("fs", "tp"),
        P("fs", "tp"),
        P("fs", "tp"),
        P("tp", "fs", None),
        P("tp", None, None),
        P("tp", "fs", None),
        P("tp", None, None),
    )
    out_specs = (
        P("fs", "tp"),
        P("tp", "fs", None),
        P("tp", None, None),
        P("fs", "tp"),
        P("fs", "tp"),
        P(None, "tp"),
    )

    def body(inputs, *rest):
        rows = inputs.shape[1] // fs
        if fs % 4 == 0 and fs >= 8 and rows % 128 == 0:
            return fast_body(fs, tp, inputs, *rest)
        return plain_body(inputs, *rest)

    return jax.shard_map(body, mesh=mesh, in_specs=in_specs, out_specs=out_specs, check_vma=False)
```
